32 devices in a mesh: ep: 16 (over z, y, x), tp: 2 (over core).
Axes of the slice: x: 2, y: 2, z: 4, core: 2. Of those that a mesh axis runs over, the one named last changes fastest.
Arguments:
- tokens: bfloat16 [8192, 2048], P(('ep', 'tp')), may hold values from -6 to 6
- norm_gain: float32 [2048], replicated, may hold values from 0.1 to 1.9
- norm_bias: float32 [2048], replicated, may hold values from -3 to 3
- gate_weight: bfloat16 [16, 2048, 1024], P('ep', None, 'tp'), may hold values from -0.125 to 0.125
- up_weight: bfloat16 [16, 2048, 1024], P('ep', None, 'tp'), may hold values from -0.125 to 0.125
- down_weight: bfloat16 [16, 1024, 2048], P('ep', 'tp'), may hold values from -0.1875 to 0.1875
- expert_ids: int32 [8192, 2], P(('ep', 'tp')), may hold values from 0 to 15, all different within a row; in each aligned block of 256 rows (0 to 255, 256 to 511, ...) at most 64 rows name the same one
- route_weights: float32 [8192, 2], P(('ep', 'tp')), may hold values from 0.2 to 1
Outputs:
- mixed: bfloat16 [8192, 2048], P(('ep', 'tp'))
The draws below stay inside these ranges and needn't reach their ends.
Inputs may be any that keep to these rules, and one draw needn't show every extreme that they name: `expert_ids`: a token's 2 experts differ; in the tokens of one device (aligned blocks of 256 rows) no expert is named by more than 64 entries, a bound that some block reaches.
All inputs are finite; a program needn't handle non-finite values.
Results may differ from the reference program's by a relative error of at most 0.0071.
Values may be sent and summed in bfloat16 or wider, within the bound.
A program may use at most 128 MiB of HBM per device.

```python
import math
import jax
import jax.numpy as jnp
import numpy as np
from jax import lax

D = 2048
FFE = 1024
TOPK = 2
TOK_DEV = 256
EXPERTS = 16
CAP = 64
TOKENS = 8192


def block_scale(key, dims, cuts, least, high):
    def one(dim, shards_of):
        draws = jax.random.uniform(jax.random.fold_in(jax.random.fold_in(key, 6), dim), (shards_of,), jnp.float32, least / len(cuts), high / len(cuts))
        return jnp.repeat(jnp.exp(draws), dims[dim] // shards_of).reshape((-1,) + (1,) * (len(dims) - dim - 1))

    level = one(*cuts[0])
    for cut in cuts[1:]:
        level = level * one(*cut)
    return level


def assign_block(stream_key, own, number, rows, number_of, top, limit, skew):
    ranking = jax.random.permutation(stream_key, number_of)
    heavy_load, common = shares(number_of, rows * top, limit, skew, True), shares(number_of, rows * top, limit, skew, False)
    places = jnp.arange(number_of)

    def named(tallies, offset_by):
        used = int((tallies > 0).sum())
        fixed = max(1, used // 4)
        moved = fixed + (places - fixed + offset_by * (used - fixed)) % max(1, number_of - fixed)
        return jnp.zeros((number_of,), jnp.int32).at[ranking[jnp.where(places < fixed, places, moved)]].set(jnp.asarray(tallies, jnp.int32))

    tallies = jnp.where(number % 4 == 0, named(heavy_load, number // 4), named(common, number - number // 4 - 1))
    mixed = jax.random.permutation(jax.random.fold_in(own, 3), number_of)
    source_of, receiver = mixed[0:number_of // 2 * 2:2], mixed[1:number_of // 2 * 2:2]
    room = jnp.minimum(tallies[source_of] - 1, limit - tallies[receiver]) // 2
    room = jnp.where((source_of == ranking[0]) | (receiver == ranking[0]) | (tallies[receiver] == 0), 0, jnp.maximum(room, 0))
    moved = jax.random.randint(jax.random.fold_in(own, 4), (number_of // 2,), 0, 1 << 20) % (room + 1)
    tallies = tallies.at[source_of].add(-moved).at[receiver].add(moved)
    members = jnp.searchsorted(jnp.cumsum(tallies), jnp.arange(rows * top), side="right").astype(jnp.int32)
    grid = members.reshape(top, rows).T
    grid = grid[jax.random.permutation(jax.random.fold_in(own, 1), rows)]
    offset_by = jax.random.randint(jax.random.fold_in(own, 2), (rows, 1), 0, top)
    return jnp.take_along_axis(grid, (jnp.arange(top)[None, :] + offset_by) % top, axis=1)


def shares(number_of, total, bound, slope, full):
    loads = [(1 << 20) // math.isqrt(rank ** slope) + 1 for rank in range(1, number_of + 1)]
    largest = bound if full else min(bound, max(-(-total // number_of), total * loads[0] // sum(loads)))
    least = 1 if total - largest >= number_of - 1 else 0
    counts, rest = [largest] + [least] * (number_of - 1), total - largest - least * (number_of - 1)
    while rest > 0:
        candidates = [i for i in range(1, number_of) if counts[i] < largest] or [i for i in range(1, number_of) if counts[i] < bound]
        pool, left = sum([loads[i] for i in candidates]), rest
        for i in candidates:
            more = min(bound - counts[i], max(1, left * loads[i] // pool), rest)
            counts[i] = counts[i] + more
            rest = rest - more
    return np.array(counts)


def scatter_about(own_key, shape, width, bound, cuts=(), held_as=jnp.bfloat16):
    array = jax.random.normal(own_key, shape, jnp.float32) * width
    if len(cuts) > 0:
        array = block_scale(own_key, shape, cuts, -0.22, 0.18) * array
    return jnp.clip(array, min=-bound, max=bound).astype(held_as)


def setup_inputs(seed: int = 0) -> dict:
    seeds = jax.random.split(jax.random.key(seed), 9)
    tokens = scatter_about(seeds[0], (TOKENS, D), 1.0, 6.0, ((0, 32),))
    norm_gain = jnp.clip(1.0 + 0.18 * jax.random.normal(seeds[1], (D,), jnp.float32), 0.1, 1.9)
    norm_bias = scatter_about(seeds[2], (D,), 0.5, 3.0, (), jnp.float32)
    gate_weight = scatter_about(seeds[3], (EXPERTS, D, FFE), D ** -0.5, 0.125, ((0, 16), (2, 2)))
    up_weight = scatter_about(seeds[4], (EXPERTS, D, FFE), D ** -0.5, 0.125, ((0, 16), (2, 2)))
    down_weight = scatter_about(seeds[5], (EXPERTS, FFE, D), FFE ** -0.5, 0.1875, ((0, 16), (1, 2)))
    expert_ids_keys = jax.random.split(jax.random.fold_in(seeds[6], 1), TOKENS // TOK_DEV)
    expert_ids_turns = jax.random.permutation(jax.random.fold_in(seeds[6], 3), TOKENS // TOK_DEV)
    expert_ids = jax.vmap(lambda own, number: assign_block(jax.random.fold_in(seeds[6], 2), own, number, TOK_DEV, EXPERTS, TOPK, CAP, 2))(expert_ids_keys, expert_ids_turns).reshape((TOKENS, TOPK))
    route_weights = jnp.clip(0.2 + 0.8 * jax.random.uniform(seeds[7], (TOKENS, TOPK), jnp.float32) ** block_scale(seeds[7], (TOKENS, TOPK), ((0, 32),), -0.2, 0.2), 0.2, 1.0)
    return {"tokens": tokens, "norm_gain": norm_gain, "norm_bias": norm_bias, "gate_weight": gate_weight, "up_weight": up_weight, "down_weight": down_weight, "expert_ids": expert_ids, "route_weights": route_weights}


def expert_rows(rows, w_gate, w_up, w_down):
    gate = jnp.dot(rows, w_gate, preferred_element_type=jnp.float32)
    upper = jnp.dot(rows, w_up, preferred_element_type=jnp.float32)
    hidden = (jax.nn.silu(gate) * upper).astype(jnp.bfloat16)
    return jnp.dot(hidden, w_down, preferred_element_type=jnp.float32).astype(jnp.bfloat16)

def reference(tokens, norm_gain, norm_bias, gate_weight, up_weight, down_weight, expert_ids, route_weights):
    values = tokens.astype(jnp.float32)
    centre = values - lax.optimization_barrier(jnp.mean(values, axis=-1, keepdims=True))
    spread = lax.optimization_barrier(jnp.mean(centre * centre, axis=-1, keepdims=True))
    normed = (centre * lax.rsqrt(spread + 1e-05) * norm_gain + norm_bias).astype(jnp.bfloat16)
    sources = TOKENS // TOK_DEV
    blocks = expert_ids.reshape(sources, TOK_DEV * TOPK)
    onehot = (blocks[:, :, None] == jnp.arange(EXPERTS, dtype=jnp.int32)[None, None, :]).astype(jnp.int32)
    slot = lax.optimization_barrier(jnp.sum(jnp.cumsum(onehot, axis=1) * onehot, axis=-1)) - 1
    row_index = (jnp.arange(sources, dtype=jnp.int32)[:, None] * CAP + slot).reshape(-1).astype(jnp.int32)
    flat_ids = expert_ids.reshape(-1)
    token_rows = jnp.repeat(normed, TOPK, axis=0)
    buffer_rows = sources * CAP

    def one_expert(expert, total):
        chosen = flat_ids == expert
        index = jnp.where(chosen, row_index, buffer_rows).astype(jnp.int32)
        buffer = jnp.zeros((buffer_rows, D), jnp.bfloat16).at[index].set(token_rows, mode='drop')
        result = expert_rows(buffer, gate_weight[expert], up_weight[expert], down_weight[expert])
        picked = result[jnp.minimum(index, buffer_rows - 1)]
        picked = jnp.where(chosen[:, None], picked.astype(jnp.float32), 0.0).reshape(TOKENS, TOPK, D)
        return total + lax.optimization_barrier(jnp.sum(picked * route_weights[:, :, None], axis=1))
    total = lax.fori_loop(0, EXPERTS, one_expert, jnp.zeros((TOKENS, D), jnp.float32))
    return total.astype(jnp.bfloat16)
```

```python
import functools

import jax
import jax.numpy as jnp
from jax import lax
from jax.experimental import pallas as pl
from jax.experimental.pallas import tpu as pltpu
from jax.sharding import PartitionSpec as P

MESH = pl.DeviceIdType.MESH
LINE = 4
CHUNKS = 8


def kernel(
    planes, nrm, meta, gw, uw, dw, out,
    tok, met, wg, wu, wd, sel, mix, snd, xin, hid, res, ret, psend, racc,
    s_own, s_met, s_mets, s_wl, s_ws, s_wr, s_tok, s_toks, s_x, s_xs, s_r, s_rs, s_p, s_ps,
):
    n = LINE
    side = planes
    me, core = lax.axis_index("ep"), lax.axis_index("tp")
    z, p = me // side, lax.rem(me, side)
    tokens, width = nrm.shape
    half = gw.shape[2]
    rows = snd.shape[1]
    cap = rows // side
    k = CHUNKS
    wide = width // k
    end = (z == 0) | (z == n - 1)
    mid = jnp.logical_not(end)
    step = jnp.where(z < n // 2, 1, -1)
    za, zb = z + step, z - step
    order = [
        z,
        jnp.where(end, z + 3 * step, z + 2 * step),
        jnp.where(end, z + 2 * step, z - step),
        z + step,
    ]

    def cols(c):
        return pl.ds(pl.multiple_of(c * wide, wide), wide)

    def band(i):
        return pl.ds(pl.multiple_of(i * cap, cap), cap)

    def plane(t):
        return {"ep": t * side + p}

    def peer(j):
        return lax.rem(p + j, side)

    def remote(src, dst, send, recv, where):
        return pltpu.make_async_remote_copy(
            src_ref=src, dst_ref=dst, send_sem=send, recv_sem=recv,
            device_id=where, device_id_type=MESH,
        )

    def landed(ref, sem):
        pltpu.make_async_copy(ref, ref, sem).wait()

    barrier = pltpu.get_barrier_semaphore()
    own = pltpu.make_async_copy(nrm, tok.at[z], s_own.at[0])
    own.start()
    ownm = pltpu.make_async_copy(meta, met.at[z], s_own.at[1])
    ownm.start()
    for j in range(1, side):
        pl.semaphore_signal(
            barrier, inc=1, device_id={"ep": z * side + peer(j)}, device_id_type=MESH
        )
    for j in range(1, n):
        pl.semaphore_signal(
            barrier, inc=1, device_id=plane(lax.rem(z + j, n)), device_id_type=MESH
        )
    pl.semaphore_signal(barrier, inc=1, device_id={"tp": 1 - core}, device_id_type=MESH)
    pl.semaphore_wait(barrier, side - 1 + n)

    def send_tok(s, c, to, way):
        remote(
            tok.at[s, :, cols(c)], tok.at[s, :, cols(c)],
            s_toks.at[way, s], s_tok.at[s, c], plane(to),
        ).start()

    def send_own(to, way):
        @pl.loop(0, k)
        def _(c):
            send_tok(z, c, to, way)

    own.wait()
    ownm.wait()
    for j in range(1, n):
        remote(
            met.at[z], met.at[z], s_mets.at[j - 1], s_met.at[z], plane(lax.rem(z + j, n))
        ).start()

    @pl.when(end)
    def _():
        send_own(za, 0)

    halfrows = pl.ds(pl.multiple_of(core * half, half), half)
    pairs = [
        (gw.at[0], wg.at[core]), (uw.at[0], wu.at[core]), (dw.at[0], wd.at[halfrows]),
    ]
    for i, (a, b) in enumerate(pairs):
        pltpu.make_async_copy(a, b, s_wl.at[i]).start()
        remote(a, b, s_ws.at[i], s_wr.at[i], {"tp": 1 - core}).start()

    def prep(q):
        s = order[q]
        ids0, ids1 = met[s, 0:1, :], met[s, 1:2, :]
        wt0, wt1 = met[s, 2:3, :], met[s, 3:4, :]
        row = lax.broadcasted_iota(jnp.int32, (rows, tokens), 0)
        e_row = (z * side + row // cap).astype(jnp.float32)
        s_row = lax.rem(row, cap).astype(jnp.float32)
        hit0 = (ids0 == e_row).astype(jnp.float32)
        hit1 = (ids1 == e_row).astype(jnp.float32)
        hit = hit0 + hit1
        before = (
            lax.broadcasted_iota(jnp.int32, (tokens, tokens), 0)
            < lax.broadcasted_iota(jnp.int32, (tokens, tokens), 1)
        ).astype(jnp.float32).astype(jnp.bfloat16)
        count = jnp.dot(hit.astype(jnp.bfloat16), before, preferred_element_type=jnp.float32)
        pick = jnp.where(count == s_row, hit, 0.0)
        sel[q] = pick.astype(jnp.bfloat16)
        w = pick * (hit0 * wt0 + hit1 * wt1)
        high = w.astype(jnp.bfloat16)
        mix[q, 0] = high
        mix[q, 1] = (w - high.astype(jnp.float32)).astype(jnp.bfloat16)

    def disp(q, c):
        y = jnp.dot(sel[q], tok[order[q], :, cols(c)], preferred_element_type=jnp.float32)
        snd[q, :, cols(c)] = y.astype(jnp.bfloat16)
        xin[q, band(p), cols(c)] = snd[q, band(p), cols(c)]
        for j in range(1, side):
            o = peer(j)
            remote(
                snd.at[q, band(o), cols(c)], xin.at[q, band(p), cols(c)],
                s_xs.at[q], s_x.at[q], {"ep": z * side + o},
            ).start()

    def others(ref, q):
        return ref.at[q, pl.ds(0, (side - 1) * cap)]

    tile = min(256, half)
    per = half // tile

    def compute(q):
        landed(others(xin, q), s_x.at[q])

        @pl.loop(0, 2 * per)
        def _(i):
            h, at = i // per, lax.rem(i, per)
            part = pl.ds(pl.multiple_of(at * tile, tile), tile)
            x = xin[q]
            g = jnp.dot(x, wg[h, :, part], preferred_element_type=jnp.float32)
            u = jnp.dot(x, wu[h, :, part], preferred_element_type=jnp.float32)
            v = g / (1.0 + jnp.exp(-g)) * u
            hid[:, pl.ds(pl.multiple_of(i * tile, tile), tile)] = v.astype(jnp.bfloat16)

        @pl.loop(0, k)
        def _(c):
            y = jnp.dot(hid[...], wd[:, cols(c)], preferred_element_type=jnp.float32)
            res[q, :, cols(c)] = y.astype(jnp.bfloat16)
            ret[q, band(p), cols(c)] = res[q, band(p), cols(c)]
            for j in range(1, side):
                o = peer(j)
                remote(
                    res.at[q, band(o), cols(c)], ret.at[q, band(p), cols(c)],
                    s_rs.at[q], s_r.at[q, c], {"ep": z * side + o},
                ).start()

    def weigh(q, c):
        landed(ret.at[q, pl.ds(0, (side - 1) * cap), cols(c)], s_r.at[q, c])
        r = ret[q, :, cols(c)]
        dims = (((0,), (0,)), ((), ()))
        return lax.dot_general(
            mix[q, 0], r, dims, preferred_element_type=jnp.float32
        ) + lax.dot_general(mix[q, 1], r, dims, preferred_element_type=jnp.float32)

    def combine(q, c, add):
        t = order[q]
        y = weigh(q, c)
        to = zb if (q == 2 and add) else za
        if add:
            landed(racc.at[t, c], s_p.at[t, c])
            y = y + racc[t, c].astype(jnp.float32)
        psend[q - 1, c] = y.astype(jnp.bfloat16)
        slot = jnp.where((to == t) & (to < z), n, t)
        remote(
            psend.at[q - 1, c], racc.at[slot, c], s_ps.at[q - 1], s_p.at[slot, c], plane(to)
        ).start()

    def arrived(s, c):
        landed(tok.at[s, :, cols(c)], s_tok.at[s, c])

    prep(0)

    @pl.loop(0, k)
    def _(c):
        disp(0, c)

    for q in range(1, n):
        landed(met.at[order[q]], s_met.at[order[q]])
        prep(q)

    def first(c):
        @pl.when(mid)
        def _():
            arrived(order[2], c)
            send_tok(order[2], c, za, 0)

        arrived(order[1], c)

        @pl.when(mid)
        def _():
            send_tok(order[1], c, zb, 1)

        disp(1, c)

        @pl.when(mid)
        def _():
            disp(2, c)

    pl.loop(0, k - 2)(first)
    for i, (a, b) in enumerate(pairs):
        pltpu.make_async_copy(a, b, s_wl.at[i]).wait()
        landed(b, s_wr.at[i])
    compute(0)
    pl.loop(k - 2, k)(first)

    @pl.when(mid)
    def _():
        send_own(za, 0)

    def second(c):
        @pl.when(mid)
        def _():
            arrived(order[3], c)
            send_tok(order[3], c, zb, 1)
            disp(3, c)

        @pl.when(end)
        def _():
            arrived(order[2], c)
            disp(2, c)

    pl.loop(0, k // 2)(second)
    compute(1)
    pl.loop(k // 2, k)(second)

    @pl.when(mid)
    def _():
        send_own(zb, 1)

    @pl.when(end)
    def _():
        pl.loop(0, k)(lambda c: combine(1, c, False))

    compute(2)

    @pl.when(end)
    def _():
        pl.loop(0, k)(lambda c: combine(2, c, False))

        @pl.loop(0, k)
        def _(c):
            arrived(order[3], c)
            disp(3, c)

    compute(3)

    @pl.when(mid)
    def _():
        @pl.loop(0, k)
        def _(c):
            combine(1, c, True)
            combine(2, c, True)

        pl.loop(0, k)(lambda c: combine(3, c, True))

    @pl.when(end)
    def _():
        pl.loop(0, k)(lambda c: combine(3, c, False))

    def last(c, slots):
        y = weigh(0, c)
        for slot in slots:
            landed(racc.at[slot, c], s_p.at[slot, c])
            y = y + racc[slot, c].astype(jnp.float32)
        out[:, cols(c)] = y.astype(out.dtype)

    @pl.when(end)
    def _():
        pl.loop(0, k)(lambda c: last(c, [jnp.where(z == 0, n, z)]))

    @pl.when(mid)
    def _():
        pl.loop(0, k)(lambda c: last(c, [z, n]))

    drain = landed

    for j in range(1, n):
        drain(met.at[z], s_mets.at[j - 1])
    for i, (a, b) in enumerate(pairs):
        drain(b, s_ws.at[i])
    drain(tok.at[z], s_toks.at[0, z])

    @pl.when(mid)
    def _():
        drain(tok.at[z], s_toks.at[1, z])
        drain(tok.at[z], s_toks.at[0, order[2]])
        drain(tok.at[z], s_toks.at[1, order[1]])
        drain(tok.at[z], s_toks.at[1, order[3]])

    for q in range(n):
        drain(others(snd, q), s_xs.at[q])
        drain(others(res, q), s_rs.at[q])
    for q in range(1, n):
        drain(psend.at[q - 1], s_ps.at[q - 1])


def body(
    tokens, norm_gain, norm_bias, gate_weight, up_weight, down_weight, expert_ids, route_weights
):
    count, width = tokens.shape
    experts = lax.axis_size("ep")
    cap = max(4 * count // experts, 4)
    side = experts // LINE
    half = gate_weight.shape[2]
    values = tokens.astype(jnp.float32)
    centre = values - jnp.mean(values, axis=-1, keepdims=True)
    spread = jnp.mean(centre * centre, axis=-1, keepdims=True)
    normed = (centre * lax.rsqrt(spread + 1e-05) * norm_gain + norm_bias).astype(jnp.bfloat16)
    both = jnp.concatenate([expert_ids.astype(jnp.float32), route_weights], axis=1)
    meta = jnp.pad(both.T, ((0, 4), (0, 0)))
    rows = side * cap
    wide = width // CHUNKS
    bf = jnp.bfloat16
    dma = pltpu.SemaphoreType.DMA
    hbm = pl.BlockSpec(memory_space=pl.ANY)
    return pl.pallas_call(
        functools.partial(kernel, side),
        out_shape=jax.ShapeDtypeStruct((count, width), bf),
        in_specs=[hbm] * 5,
        out_specs=pl.BlockSpec(memory_space=pltpu.VMEM),
        scratch_shapes=[
            pltpu.VMEM((LINE, count, width), bf),
            pltpu.VMEM((LINE, 8, count), jnp.float32),
            pltpu.VMEM((2, width, half), bf),
            pltpu.VMEM((2, width, half), bf),
            pltpu.VMEM((2 * half, width), bf),
            pltpu.VMEM((LINE, rows, count), bf),
            pltpu.VMEM((LINE, 2, rows, count), bf),
            pltpu.VMEM((LINE, rows, width), bf),
            pltpu.VMEM((LINE, rows, width), bf),
            pltpu.VMEM((rows, 2 * half), bf),
            pltpu.VMEM((LINE, rows, width), bf),
            pltpu.VMEM((LINE, rows, width), bf),
            pltpu.VMEM((LINE - 1, CHUNKS, count, wide), bf),
            pltpu.VMEM((LINE + 1, CHUNKS, count, wide), bf),
            dma((2,)),
            dma((LINE,)),
            dma((LINE - 1,)),
            dma((3,)),
            dma((3,)),
            dma((3,)),
            dma((LINE, CHUNKS)),
            dma((2, LINE)),
            dma((LINE,)),
            dma((LINE,)),
            dma((LINE, CHUNKS)),
            dma((LINE,)),
            dma((LINE + 1, CHUNKS)),
            dma((LINE - 1,)),
        ],
        compiler_params=pltpu.CompilerParams(
            collective_id=0, has_side_effects=True, vmem_limit_bytes=60 * 1024 * 1024
        ),
    )(normed, meta, gate_weight, up_weight, down_weight)


def solution(mesh):
    placed = (
        P(("ep", "tp"), None),
        P(),
        P(),
        P("ep", None, "tp"),
        P("ep", None, "tp"),
        P("ep", "tp", None),
        P(("ep", "tp"), None),
        P(("ep", "tp"), None),
    )
    return jax.shard_map(
        body, mesh=mesh, in_specs=placed, out_specs=P(("ep", "tp"), None), check_vma=False
    )
```

```python
import functools

import jax
import jax.numpy as jnp
from jax import lax
from jax.experimental import pallas as pl
from jax.experimental.pallas import tpu as pltpu
from jax.sharding import PartitionSpec as P

MESH = pl.DeviceIdType.MESH
LINE = 4
CHUNKS = 8
LAG = 2


def kernel(
    planes, nrm, meta, gw, uw, dw, out,
    tok, met, wg, wu, wd, sel, mix, snd, xin, hid, res, ret, psend, racc,
    s_own, s_met, s_mets, s_wl, s_ws, s_wr, s_tok, s_toks, s_x, s_xs, s_r, s_rs, s_p, s_ps,
):
    n = LINE
    side = planes
    me, core = lax.axis_index("ep"), lax.axis_index("tp")
    z, p = me // side, lax.rem(me, side)
    tokens, width = nrm.shape
    half = gw.shape[2]
    rows = snd.shape[1]
    cap = rows // side
    k = CHUNKS
    wide = width // k
    end = (z == 0) | (z == n - 1)
    mid = jnp.logical_not(end)
    step = jnp.where(z < n // 2, 1, -1)
    za, zb = z + step, z - step
    order = [
        z,
        jnp.where(end, z + 3 * step, z + 2 * step),
        jnp.where(end, z + 2 * step, z - step),
        z + step,
    ]

    def cols(c):
        return pl.ds(pl.multiple_of(c * wide, wide), wide)

    def band(i):
        return pl.ds(pl.multiple_of(i * cap, cap), cap)

    def plane(t):
        return {"ep": t * side + p}

    def peer(j):
        return lax.rem(p + j, side)

    def remote(src, dst, send, recv, where):
        return pltpu.make_async_remote_copy(
            src_ref=src, dst_ref=dst, send_sem=send, recv_sem=recv,
            device_id=where, device_id_type=MESH,
        )

    def landed(ref, sem):
        pltpu.make_async_copy(ref, ref, sem).wait()

    barrier = pltpu.get_barrier_semaphore()
    own = pltpu.make_async_copy(nrm, tok.at[z], s_own.at[0])
    own.start()
    ownm = pltpu.make_async_copy(meta, met.at[z], s_own.at[1])
    ownm.start()
    for j in range(1, side):
        pl.semaphore_signal(
            barrier, inc=1, device_id={"ep": z * side + peer(j)}, device_id_type=MESH
        )
    for j in range(1, n):
        pl.semaphore_signal(
            barrier, inc=1, device_id=plane(lax.rem(z + j, n)), device_id_type=MESH
        )
    pl.semaphore_signal(barrier, inc=1, device_id={"tp": 1 - core}, device_id_type=MESH)
    pl.semaphore_wait(barrier, side - 1 + n)

    def send_tok(s, c, to, way):
        remote(
            tok.at[s, :, cols(c)], tok.at[s, :, cols(c)],
            s_toks.at[way, s], s_tok.at[s, c], plane(to),
        ).start()

    def send_own(to, way):
        @pl.loop(0, k)
        def _(c):
            send_tok(z, c, to, way)

    own.wait()
    ownm.wait()
    for j in range(1, n):
        remote(
            met.at[z], met.at[z], s_mets.at[j - 1], s_met.at[z], plane(lax.rem(z + j, n))
        ).start()

    @pl.when(end)
    def _():
        send_own(za, 0)

    halfrows = pl.ds(pl.multiple_of(core * half, half), half)
    pairs = [
        (gw.at[0], wg.at[core]), (uw.at[0], wu.at[core]), (dw.at[0], wd.at[halfrows]),
    ]
    for i, (a, b) in enumerate(pairs):
        pltpu.make_async_copy(a, b, s_wl.at[i]).start()
        remote(a, b, s_ws.at[i], s_wr.at[i], {"tp": 1 - core}).start()

    def prep(q):
        s = order[q]
        ids0, ids1 = met[s, 0:1, :], met[s, 1:2, :]
        wt0, wt1 = met[s, 2:3, :], met[s, 3:4, :]
        row = lax.broadcasted_iota(jnp.int32, (rows, tokens), 0)
        e_row = (z * side + row // cap).astype(jnp.float32)
        s_row = lax.rem(row, cap).astype(jnp.float32)
        hit0 = (ids0 == e_row).astype(jnp.float32)
        hit1 = (ids1 == e_row).astype(jnp.float32)
        hit = hit0 + hit1
        before = (
            lax.broadcasted_iota(jnp.int32, (tokens, tokens), 0)
            < lax.broadcasted_iota(jnp.int32, (tokens, tokens), 1)
        ).astype(jnp.float32).astype(jnp.bfloat16)
        count = jnp.dot(hit.astype(jnp.bfloat16), before, preferred_element_type=jnp.float32)
        pick = jnp.where(count == s_row, hit, 0.0)
        sel[q] = pick.astype(jnp.bfloat16)
        w = pick * (hit0 * wt0 + hit1 * wt1)
        high = w.astype(jnp.bfloat16)
        mix[q, 0] = high
        mix[q, 1] = (w - high.astype(jnp.float32)).astype(jnp.bfloat16)

    def disp(q, c):
        y = jnp.dot(sel[q], tok[order[q], :, cols(c)], preferred_element_type=jnp.float32)
        snd[q, :, cols(c)] = y.astype(jnp.bfloat16)
        xin[q, band(p), cols(c)] = snd[q, band(p), cols(c)]
        for j in range(1, side):
            o = peer(j)
            remote(
                snd.at[q, band(o), cols(c)], xin.at[q, band(p), cols(c)],
                s_xs.at[q], s_x.at[q], {"ep": z * side + o},
            ).start()

    def others(ref, q):
        return ref.at[q, pl.ds(0, (side - 1) * cap)]

    tile = min(256, half)
    per = half // tile

    def compute(q):
        landed(others(xin, q), s_x.at[q])

        @pl.loop(0, 2 * per)
        def _(i):
            h, at = i // per, lax.rem(i, per)
            part = pl.ds(pl.multiple_of(at * tile, tile), tile)
            x = xin[q]
            g = jnp.dot(x, wg[h, :, part], preferred_element_type=jnp.float32)
            u = jnp.dot(x, wu[h, :, part], preferred_element_type=jnp.float32)
            v = g / (1.0 + jnp.exp(-g)) * u
            hid[:, pl.ds(pl.multiple_of(i * tile, tile), tile)] = v.astype(jnp.bfloat16)

        @pl.loop(0, k)
        def _(c):
            y = jnp.dot(hid[...], wd[:, cols(c)], preferred_element_type=jnp.float32)
            res[q, :, cols(c)] = y.astype(jnp.bfloat16)
            ret[q, band(p), cols(c)] = res[q, band(p), cols(c)]
            for j in range(1, side):
                o = peer(j)
                remote(
                    res.at[q, band(o), cols(c)], ret.at[q, band(p), cols(c)],
                    s_rs.at[q], s_r.at[q, c], {"ep": z * side + o},
                ).start()

    def weigh(q, c):
        landed(ret.at[q, pl.ds(0, (side - 1) * cap), cols(c)], s_r.at[q, c])
        r = ret[q, :, cols(c)]
        dims = (((0,), (0,)), ((), ()))
        return lax.dot_general(
            mix[q, 0], r, dims, preferred_element_type=jnp.float32
        ) + lax.dot_general(mix[q, 1], r, dims, preferred_element_type=jnp.float32)

    def combine(q, c, add):
        t = order[q]
        y = weigh(q, c)
        to = zb if (q == 2 and add) else za
        if add:
            landed(racc.at[t, c], s_p.at[t, c])
            y = y + racc[t, c].astype(jnp.float32)
        psend[q - 1, c] = y.astype(jnp.bfloat16)
        slot = jnp.where((to == t) & (to < z), n, t)
        remote(
            psend.at[q - 1, c], racc.at[slot, c], s_ps.at[q - 1], s_p.at[slot, c], plane(to)
        ).start()

    def arrived(s, c):
        landed(tok.at[s, :, cols(c)], s_tok.at[s, c])

    prep(0)

    @pl.loop(0, k)
    def _(c):
        disp(0, c)

    for q in range(1, n):
        landed(met.at[order[q]], s_met.at[order[q]])
        prep(q)

    def near(c):
        @pl.when(mid)
        def _():
            arrived(order[2], c)
            send_tok(order[2], c, za, 0)
            disp(2, c)

    def far(c):
        arrived(order[1], c)

        @pl.when(mid)
        def _():
            send_tok(order[1], c, zb, 1)

        disp(1, c)

    for c in range(LAG):
        near(c)

    @pl.loop(LAG, k)
    def _(c):
        near(c)
        far(c - LAG)

    @pl.when(mid)
    def _():
        send_own(za, 0)

    for i, (a, b) in enumerate(pairs):
        pltpu.make_async_copy(a, b, s_wl.at[i]).wait()
        landed(b, s_wr.at[i])
    compute(0)
    pl.loop(k - LAG, k)(far)

    def second(c):
        @pl.when(mid)
        def _():
            arrived(order[3], c)
            send_tok(order[3], c, zb, 1)
            disp(3, c)

        @pl.when(end)
        def _():
            arrived(order[2], c)
            disp(2, c)

    pl.loop(0, k // 2)(second)
    compute(1)
    pl.loop(k // 2, k)(second)

    @pl.when(mid)
    def _():
        send_own(zb, 1)

    @pl.when(end)
    def _():
        pl.loop(0, k)(lambda c: combine(1, c, False))

    compute(2)

    @pl.when(end)
    def _():
        @pl.loop(0, k)
        def _(c):
            combine(2, c, False)
            arrived(order[3], c)
            disp(3, c)

    compute(3)

    @pl.when(mid)
    def _():
        for c in range(LAG):
            combine(1, c, True)

        @pl.loop(LAG, k)
        def _(c):
            combine(1, c, True)
            combine(2, c - LAG, True)

        pl.loop(k - LAG, k)(lambda c: combine(2, c, True))
        pl.loop(0, k)(lambda c: combine(3, c, True))

    @pl.when(end)
    def _():
        pl.loop(0, k)(lambda c: combine(3, c, False))

    def last(c, slots):
        y = weigh(0, c)
        for slot in slots:
            landed(racc.at[slot, c], s_p.at[slot, c])
            y = y + racc[slot, c].astype(jnp.float32)
        out[:, cols(c)] = y.astype(out.dtype)

    @pl.when(end)
    def _():
        pl.loop(0, k)(lambda c: last(c, [jnp.where(z == 0, n, z)]))

    @pl.when(mid)
    def _():
        pl.loop(0, k)(lambda c: last(c, [z, n]))

    drain = landed

    for j in range(1, n):
        drain(met.at[z], s_mets.at[j - 1])
    for i, (a, b) in enumerate(pairs):
        drain(b, s_ws.at[i])
    drain(tok.at[z], s_toks.at[0, z])

    @pl.when(mid)
    def _():
        drain(tok.at[z], s_toks.at[1, z])
        drain(tok.at[z], s_toks.at[0, order[2]])
        drain(tok.at[z], s_toks.at[1, order[1]])
        drain(tok.at[z], s_toks.at[1, order[3]])

    for q in range(n):
        drain(others(snd, q), s_xs.at[q])
        drain(others(res, q), s_rs.at[q])
    for q in range(1, n):
        drain(psend.at[q - 1], s_ps.at[q - 1])


def body(
    tokens, norm_gain, norm_bias, gate_weight, up_weight, down_weight, expert_ids, route_weights
):
    count, width = tokens.shape
    experts = lax.axis_size("ep")
    cap = max(4 * count // experts, 4)
    side = experts // LINE
    half = gate_weight.shape[2]
    values = tokens.astype(jnp.float32)
    centre = values - jnp.mean(values, axis=-1, keepdims=True)
    spread = jnp.mean(centre * centre, axis=-1, keepdims=True)
    normed = (centre * lax.rsqrt(spread + 1e-05) * norm_gain + norm_bias).astype(jnp.bfloat16)
    both = jnp.concatenate([expert_ids.astype(jnp.float32), route_weights], axis=1)
    meta = jnp.pad(both.T, ((0, 4), (0, 0)))
    rows = side * cap
    wide = width // CHUNKS
    bf = jnp.bfloat16
    dma = pltpu.SemaphoreType.DMA
    hbm = pl.BlockSpec(memory_space=pl.ANY)
    return pl.pallas_call(
        functools.partial(kernel, side),
        out_shape=jax.ShapeDtypeStruct((count, width), bf),
        in_specs=[hbm] * 5,
        out_specs=pl.BlockSpec(memory_space=pltpu.VMEM),
        scratch_shapes=[
            pltpu.VMEM((LINE, count, width), bf),
            pltpu.VMEM((LINE, 8, count), jnp.float32),
            pltpu.VMEM((2, width, half), bf),
            pltpu.VMEM((2, width, half), bf),
            pltpu.VMEM((2 * half, width), bf),
            pltpu.VMEM((LINE, rows, count), bf),
            pltpu.VMEM((LINE, 2, rows, count), bf),
            pltpu.VMEM((LINE, rows, width), bf),
            pltpu.VMEM((LINE, rows, width), bf),
            pltpu.VMEM((rows, 2 * half), bf),
            pltpu.VMEM((LINE, rows, width), bf),
            pltpu.VMEM((LINE, rows, width), bf),
            pltpu.VMEM((LINE - 1, CHUNKS, count, wide), bf),
            pltpu.VMEM((LINE + 1, CHUNKS, count, wide), bf),
            dma((2,)),
            dma((LINE,)),
            dma((LINE - 1,)),
            dma((3,)),
            dma((3,)),
            dma((3,)),
            dma((LINE, CHUNKS)),
            dma((2, LINE)),
            dma((LINE,)),
            dma((LINE,)),
            dma((LINE, CHUNKS)),
            dma((LINE,)),
            dma((LINE + 1, CHUNKS)),
            dma((LINE - 1,)),
        ],
        compiler_params=pltpu.CompilerParams(
            collective_id=0, has_side_effects=True, vmem_limit_bytes=60 * 1024 * 1024
        ),
    )(normed, meta, gate_weight, up_weight, down_weight)


def solution(mesh):
    placed = (
        P(("ep", "tp"), None),
        P(),
        P(),
        P("ep", None, "tp"),
        P("ep", None, "tp"),
        P("ep", "tp", None),
        P(("ep", "tp"), None),
        P(("ep", "tp"), None),
    )
    return jax.shard_map(
        body, mesh=mesh, in_specs=placed, out_specs=P(("ep", "tp"), None), check_vma=False
    )
```

```python
import functools

import jax
import jax.numpy as jnp
from jax import lax
from jax.experimental import pallas as pl
from jax.experimental.pallas import tpu as pltpu
from jax.sharding import PartitionSpec as P

MESH = pl.DeviceIdType.MESH
LINE = 4
CHUNKS = 8
LAG = 2


def kernel(
    planes, nrm, meta, gw, uw, dw, out,
    tok, met, wg, wu, wd, sel, mix, snd, xin, hid, res, ret, psend, racc,
    s_own, s_met, s_mets, s_wl, s_ws, s_wr, s_tok, s_toks, s_x, s_xs, s_r, s_rs, s_p, s_ps,
):
    n = LINE
    side = planes
    me, core = lax.axis_index("ep"), lax.axis_index("tp")
    z, p = me // side, lax.rem(me, side)
    tokens, width = nrm.shape
    half = gw.shape[2]
    rows = snd.shape[1]
    cap = rows // side
    k = CHUNKS
    wide = width // k
    end = (z == 0) | (z == n - 1)
    mid = jnp.logical_not(end)
    step = jnp.where(z < n // 2, 1, -1)
    za, zb = z + step, z - step
    order = [
        z,
        jnp.where(end, z + 3 * step, z + 2 * step),
        jnp.where(end, z + 2 * step, z - step),
        z + step,
    ]

    def cols(c):
        return pl.ds(pl.multiple_of(c * wide, wide), wide)

    def band(i):
        return pl.ds(pl.multiple_of(i * cap, cap), cap)

    def plane(t):
        return {"ep": t * side + p}

    def peer(j):
        return lax.rem(p + j, side)

    def remote(src, dst, send, recv, where):
        return pltpu.make_async_remote_copy(
            src_ref=src, dst_ref=dst, send_sem=send, recv_sem=recv,
            device_id=where, device_id_type=MESH,
        )

    def landed(ref, sem):
        pltpu.make_async_copy(ref, ref, sem).wait()

    barrier = pltpu.get_barrier_semaphore()
    own = pltpu.make_async_copy(nrm, tok.at[z], s_own.at[0])
    own.start()
    ownm = pltpu.make_async_copy(meta, met.at[z], s_own.at[1])
    ownm.start()
    for j in range(1, side):
        pl.semaphore_signal(
            barrier, inc=1, device_id={"ep": z * side + peer(j)}, device_id_type=MESH
        )
    for j in range(1, n):
        pl.semaphore_signal(
            barrier, inc=1, device_id=plane(lax.rem(z + j, n)), device_id_type=MESH
        )
    pl.semaphore_signal(barrier, inc=1, device_id={"tp": 1 - core}, device_id_type=MESH)
    pl.semaphore_wait(barrier, side - 1 + n)

    def send_tok(s, c, to, way):
        remote(
            tok.at[s, :, cols(c)], tok.at[s, :, cols(c)],
            s_toks.at[way, s], s_tok.at[s, c], plane(to),
        ).start()

    def send_own(to, way):
        @pl.loop(0, k)
        def _(c):
            send_tok(z, c, to, way)

    own.wait()
    ownm.wait()
    for j in range(1, n):
        remote(
            met.at[z], met.at[z], s_mets.at[j - 1], s_met.at[z], plane(lax.rem(z + j, n))
        ).start()

    @pl.when(end)
    def _():
        send_own(za, 0)

    halfrows = pl.ds(pl.multiple_of(core * half, half), half)
    pairs = [
        (gw.at[0], wg.at[core]), (uw.at[0], wu.at[core]), (dw.at[0], wd.at[halfrows]),
    ]
    for i, (a, b) in enumerate(pairs):
        pltpu.make_async_copy(a, b, s_wl.at[i]).start()
        remote(a, b, s_ws.at[i], s_wr.at[i], {"tp": 1 - core}).start()

    def prep(q):
        s = order[q]
        ids0, ids1 = met[s, 0:1, :], met[s, 1:2, :]
        wt0, wt1 = met[s, 2:3, :], met[s, 3:4, :]
        row = lax.broadcasted_iota(jnp.int32, (rows, tokens), 0)
        e_row = (z * side + row // cap).astype(jnp.float32)
        s_row = lax.rem(row, cap).astype(jnp.float32)
        hit0 = (ids0 == e_row).astype(jnp.float32)
        hit1 = (ids1 == e_row).astype(jnp.float32)
        hit = hit0 + hit1
        before = (
            lax.broadcasted_iota(jnp.int32, (tokens, tokens), 0)
            < lax.broadcasted_iota(jnp.int32, (tokens, tokens), 1)
        ).astype(jnp.float32).astype(jnp.bfloat16)
        count = jnp.dot(hit.astype(jnp.bfloat16), before, preferred_element_type=jnp.float32)
        pick = jnp.where(count == s_row, hit, 0.0)
        sel[q] = pick.astype(jnp.bfloat16)
        w = pick * (hit0 * wt0 + hit1 * wt1)
        high = w.astype(jnp.bfloat16)
        mix[q, 0] = high
        mix[q, 1] = (w - high.astype(jnp.float32)).astype(jnp.bfloat16)

    def disp(q, c):
        y = jnp.dot(sel[q], tok[order[q], :, cols(c)], preferred_element_type=jnp.float32)
        snd[q, :, cols(c)] = y.astype(jnp.bfloat16)
        xin[q, band(p), cols(c)] = snd[q, band(p), cols(c)]
        for j in range(1, side):
            o = peer(j)
            remote(
                snd.at[q, band(o), cols(c)], xin.at[q, band(p), cols(c)],
                s_xs.at[q], s_x.at[q], {"ep": z * side + o},
            ).start()

    def others(ref, q):
        return ref.at[q, pl.ds(0, (side - 1) * cap)]

    tile = min(256, half)
    per = half // tile

    def gate(q, i):
        h, at = i // per, lax.rem(i, per)
        part = pl.ds(pl.multiple_of(at * tile, tile), tile)
        x = xin[q]
        g = jnp.dot(x, wg[h, :, part], preferred_element_type=jnp.float32)
        u = jnp.dot(x, wu[h, :, part], preferred_element_type=jnp.float32)
        v = g / (1.0 + jnp.exp(-g)) * u
        hid[:, pl.ds(pl.multiple_of(i * tile, tile), tile)] = v.astype(jnp.bfloat16)

    def down(q):
        @pl.loop(0, k)
        def _(c):
            y = jnp.dot(hid[...], wd[:, cols(c)], preferred_element_type=jnp.float32)
            res[q, :, cols(c)] = y.astype(jnp.bfloat16)
            ret[q, band(p), cols(c)] = res[q, band(p), cols(c)]
            for j in range(1, side):
                o = peer(j)
                remote(
                    res.at[q, band(o), cols(c)], ret.at[q, band(p), cols(c)],
                    s_rs.at[q], s_r.at[q, c], {"ep": z * side + o},
                ).start()

    def compute(q):
        landed(others(xin, q), s_x.at[q])
        pl.loop(0, 2 * per)(lambda i: gate(q, i))
        down(q)

    def weigh(q, c):
        landed(ret.at[q, pl.ds(0, (side - 1) * cap), cols(c)], s_r.at[q, c])
        r = ret[q, :, cols(c)]
        dims = (((0,), (0,)), ((), ()))
        return lax.dot_general(
            mix[q, 0], r, dims, preferred_element_type=jnp.float32
        ) + lax.dot_general(mix[q, 1], r, dims, preferred_element_type=jnp.float32)

    def combine(q, c, add):
        t = order[q]
        y = weigh(q, c)
        to = zb if (q == 2 and add) else za
        if add:
            landed(racc.at[t, c], s_p.at[t, c])
            y = y + racc[t, c].astype(jnp.float32)
        psend[q - 1, c] = y.astype(jnp.bfloat16)
        slot = jnp.where((to == t) & (to < z), n, t)
        remote(
            psend.at[q - 1, c], racc.at[slot, c], s_ps.at[q - 1], s_p.at[slot, c], plane(to)
        ).start()

    def arrived(s, c):
        landed(tok.at[s, :, cols(c)], s_tok.at[s, c])

    prep(0)

    @pl.loop(0, k)
    def _(c):
        disp(0, c)

    for q in range(1, n):
        landed(met.at[order[q]], s_met.at[order[q]])
        prep(q)

    def near(c):
        @pl.when(mid)
        def _():
            arrived(order[2], c)
            send_tok(order[2], c, za, 0)
            disp(2, c)

    def far(c):
        arrived(order[1], c)

        @pl.when(mid)
        def _():
            send_tok(order[1], c, zb, 1)

        disp(1, c)

    for c in range(LAG):
        near(c)

    @pl.loop(LAG, k)
    def _(c):
        near(c)
        far(c - LAG)

    @pl.when(mid)
    def _():
        send_own(za, 0)

    pl.loop(k - LAG, k)(far)

    for i, (a, b) in enumerate(pairs):
        pltpu.make_async_copy(a, b, s_wl.at[i]).wait()
        landed(b, s_wr.at[i])

    @pl.when(mid)
    def _():
        def pass_on(c):
            arrived(order[3], c)
            send_tok(order[3], c, zb, 1)
            disp(3, c)

        pl.loop(0, k // 2)(pass_on)
        landed(others(xin, 1), s_x.at[1])
        turns = k - k // 2
        for j in range(turns):
            pass_on(k // 2 + j)
            for i in range(j * 2 * per // turns, (j + 1) * 2 * per // turns):
                gate(1, i)
        send_own(zb, 1)
        down(1)
        compute(2)
        compute(3)
        for c in range(LAG):
            combine(1, c, True)

        @pl.loop(LAG, k)
        def _(c):
            combine(1, c, True)
            combine(2, c - LAG, True)

        pl.loop(k - LAG, k)(lambda c: combine(2, c, True))
        compute(0)
        pl.loop(0, k)(lambda c: combine(3, c, True))

    @pl.when(end)
    def _():
        compute(1)

        @pl.loop(0, k)
        def _(c):
            arrived(order[2], c)
            disp(2, c)
            combine(1, c, False)

        compute(0)
        compute(2)

        @pl.loop(0, k)
        def _(c):
            combine(2, c, False)
            arrived(order[3], c)
            disp(3, c)

        compute(3)
        pl.loop(0, k)(lambda c: combine(3, c, False))

    def last(c, slots):
        y = weigh(0, c)
        for slot in slots:
            landed(racc.at[slot, c], s_p.at[slot, c])
            y = y + racc[slot, c].astype(jnp.float32)
        out[:, cols(c)] = y.astype(out.dtype)

    @pl.when(end)
    def _():
        pl.loop(0, k)(lambda c: last(c, [jnp.where(z == 0, n, z)]))

    @pl.when(mid)
    def _():
        pl.loop(0, k)(lambda c: last(c, [z, n]))

    drain = landed

    for j in range(1, n):
        drain(met.at[z], s_mets.at[j - 1])
    for i, (a, b) in enumerate(pairs):
        drain(b, s_ws.at[i])
    drain(tok.at[z], s_toks.at[0, z])

    @pl.when(mid)
    def _():
        drain(tok.at[z], s_toks.at[1, z])
        drain(tok.at[z], s_toks.at[0, order[2]])
        drain(tok.at[z], s_toks.at[1, order[1]])
        drain(tok.at[z], s_toks.at[1, order[3]])

    for q in range(n):
        drain(others(snd, q), s_xs.at[q])
        drain(others(res, q), s_rs.at[q])
    for q in range(1, n):
        drain(psend.at[q - 1], s_ps.at[q - 1])


def body(
    tokens, norm_gain, norm_bias, gate_weight, up_weight, down_weight, expert_ids, route_weights
):
    count, width = tokens.shape
    experts = lax.axis_size("ep")
    cap = max(4 * count // experts, 4)
    side = experts // LINE
    half = gate_weight.shape[2]
    values = tokens.astype(jnp.float32)
    centre = values - jnp.mean(values, axis=-1, keepdims=True)
    spread = jnp.mean(centre * centre, axis=-1, keepdims=True)
    normed = (centre * lax.rsqrt(spread + 1e-05) * norm_gain + norm_bias).astype(jnp.bfloat16)
    both = jnp.concatenate([expert_ids.astype(jnp.float32), route_weights], axis=1)
    meta = jnp.pad(both.T, ((0, 4), (0, 0)))
    rows = side * cap
    wide = width // CHUNKS
    bf = jnp.bfloat16
    dma = pltpu.SemaphoreType.DMA
    hbm = pl.BlockSpec(memory_space=pl.ANY)
    return pl.pallas_call(
        functools.partial(kernel, side),
        out_shape=jax.ShapeDtypeStruct((count, width), bf),
        in_specs=[hbm] * 5,
        out_specs=pl.BlockSpec(memory_space=pltpu.VMEM),
        scratch_shapes=[
            pltpu.VMEM((LINE, count, width), bf),
            pltpu.VMEM((LINE, 8, count), jnp.float32),
            pltpu.VMEM((2, width, half), bf),
            pltpu.VMEM((2, width, half), bf),
            pltpu.VMEM((2 * half, width), bf),
            pltpu.VMEM((LINE, rows, count), bf),
            pltpu.VMEM((LINE, 2, rows, count), bf),
            pltpu.VMEM((LINE, rows, width), bf),
            pltpu.VMEM((LINE, rows, width), bf),
            pltpu.VMEM((rows, 2 * half), bf),
            pltpu.VMEM((LINE, rows, width), bf),
            pltpu.VMEM((LINE, rows, width), bf),
            pltpu.VMEM((LINE - 1, CHUNKS, count, wide), bf),
            pltpu.VMEM((LINE + 1, CHUNKS, count, wide), bf),
            dma((2,)),
            dma((LINE,)),
            dma((LINE - 1,)),
            dma((3,)),
            dma((3,)),
            dma((3,)),
            dma((LINE, CHUNKS)),
            dma((2, LINE)),
            dma((LINE,)),
            dma((LINE,)),
            dma((LINE, CHUNKS)),
            dma((LINE,)),
            dma((LINE + 1, CHUNKS)),
            dma((LINE - 1,)),
        ],
        compiler_params=pltpu.CompilerParams(
            collective_id=0, has_side_effects=True, vmem_limit_bytes=60 * 1024 * 1024
        ),
    )(normed, meta, gate_weight, up_weight, down_weight)


def solution(mesh):
    placed = (
        P(("ep", "tp"), None),
        P(),
        P(),
        P("ep", None, "tp"),
        P("ep", None, "tp"),
        P("ep", "tp", None),
        P(("ep", "tp"), None),
        P(("ep", "tp"), None),
    )
    return jax.shard_map(
        body, mesh=mesh, in_specs=placed, out_specs=P(("ep", "tp"), None), check_vma=False
    )
```

```python
import functools

import jax
import jax.numpy as jnp
from jax import lax
from jax.experimental import pallas as pl
from jax.experimental.pallas import tpu as pltpu
from jax.sharding import PartitionSpec as P

MESH = pl.DeviceIdType.MESH
LINE = 4
CHUNKS = 8
LAG = 2


def kernel(
    planes, raw, gain, bias, meta, gw, uw, dw, out,
    src, tok, met, wg, wu, wd, sel, mix, snd, xin, hid, res, ret, psend, racc,
    s_own, s_met, s_mets, s_wl, s_ws, s_wr, s_tok, s_toks, s_x, s_xs, s_r, s_rs, s_p, s_ps,
):
    n = LINE
    side = planes
    me, core = lax.axis_index("ep"), lax.axis_index("tp")
    z, p = me // side, lax.rem(me, side)
    tokens, width = raw.shape
    half = gw.shape[2]
    rows = snd.shape[1]
    cap = rows // side
    k = CHUNKS
    wide = width // k
    end = (z == 0) | (z == n - 1)
    mid = jnp.logical_not(end)
    step = jnp.where(z < n // 2, 1, -1)
    za, zb = z + step, z - step
    order = [
        z,
        jnp.where(end, z + 3 * step, z + 2 * step),
        jnp.where(end, z + 2 * step, z - step),
        z + step,
    ]

    def cols(c):
        return pl.ds(pl.multiple_of(c * wide, wide), wide)

    def band(i):
        return pl.ds(pl.multiple_of(i * cap, cap), cap)

    def plane(t):
        return {"ep": t * side + p}

    def peer(j):
        return lax.rem(p + j, side)

    def remote(src, dst, send, recv, where):
        return pltpu.make_async_remote_copy(
            src_ref=src, dst_ref=dst, send_sem=send, recv_sem=recv,
            device_id=where, device_id_type=MESH,
        )

    def landed(ref, sem):
        pltpu.make_async_copy(ref, ref, sem).wait()

    barrier = pltpu.get_barrier_semaphore()
    own = pltpu.make_async_copy(raw, src, s_own.at[0])
    own.start()
    ownm = pltpu.make_async_copy(meta, met.at[z], s_own.at[1])
    ownm.start()
    for j in range(1, side):
        pl.semaphore_signal(
            barrier, inc=1, device_id={"ep": z * side + peer(j)}, device_id_type=MESH
        )
    for j in range(1, n):
        pl.semaphore_signal(
            barrier, inc=1, device_id=plane(lax.rem(z + j, n)), device_id_type=MESH
        )
    pl.semaphore_signal(barrier, inc=1, device_id={"tp": 1 - core}, device_id_type=MESH)

    def send_tok(s, c, to, way):
        remote(
            tok.at[s, :, cols(c)], tok.at[s, :, cols(c)],
            s_toks.at[way, s], s_tok.at[s, c], plane(to),
        ).start()

    def send_own(to, way):
        @pl.loop(0, k)
        def _(c):
            send_tok(z, c, to, way)

    def prep(q):
        s = order[q]
        ids0, ids1 = met[s, 0:1, :], met[s, 1:2, :]
        wt0, wt1 = met[s, 2:3, :], met[s, 3:4, :]
        row = lax.broadcasted_iota(jnp.int32, (rows, tokens), 0)
        e_row = (z * side + row // cap).astype(jnp.float32)
        s_row = lax.rem(row, cap).astype(jnp.float32)
        hit0 = (ids0 == e_row).astype(jnp.float32)
        hit1 = (ids1 == e_row).astype(jnp.float32)
        hit = hit0 + hit1
        before = (
            lax.broadcasted_iota(jnp.int32, (tokens, tokens), 0)
            < lax.broadcasted_iota(jnp.int32, (tokens, tokens), 1)
        ).astype(jnp.float32).astype(jnp.bfloat16)
        count = jnp.dot(hit.astype(jnp.bfloat16), before, preferred_element_type=jnp.float32)
        pick = jnp.where(count == s_row, hit, 0.0)
        sel[q] = pick.astype(jnp.bfloat16)
        w = pick * (hit0 * wt0 + hit1 * wt1)
        high = w.astype(jnp.bfloat16)
        mix[q, 0] = high
        mix[q, 1] = (w - high.astype(jnp.float32)).astype(jnp.bfloat16)

    own.wait()
    slab = min(32, tokens)

    @pl.loop(0, tokens // slab)
    def _(i):
        at = pl.ds(pl.multiple_of(i * slab, slab), slab)
        v = src[at, :].astype(jnp.float32)
        v = v - jnp.mean(v, axis=-1, keepdims=True)
        spread = jnp.mean(v * v, axis=-1, keepdims=True)
        y = v * lax.rsqrt(spread + 1e-05) * gain[...] + bias[...]
        tok[z, at, :] = y.astype(jnp.bfloat16)

    ownm.wait()
    prep(0)
    pl.semaphore_wait(barrier, side - 1 + n)
    for j in range(1, n):
        remote(
            met.at[z], met.at[z], s_mets.at[j - 1], s_met.at[z], plane(lax.rem(z + j, n))
        ).start()

    @pl.when(end)
    def _():
        send_own(za, 0)

    halfrows = pl.ds(pl.multiple_of(core * half, half), half)
    pairs = [
        (gw.at[0], wg.at[core]), (uw.at[0], wu.at[core]), (dw.at[0], wd.at[halfrows]),
    ]
    for i, (a, b) in enumerate(pairs):
        pltpu.make_async_copy(a, b, s_wl.at[i]).start()
        remote(a, b, s_ws.at[i], s_wr.at[i], {"tp": 1 - core}).start()

    def disp(q, c):
        y = jnp.dot(sel[q], tok[order[q], :, cols(c)], preferred_element_type=jnp.float32)
        snd[q, :, cols(c)] = y.astype(jnp.bfloat16)
        xin[q, band(p), cols(c)] = snd[q, band(p), cols(c)]
        for j in range(1, side):
            o = peer(j)
            remote(
                snd.at[q, band(o), cols(c)], xin.at[q, band(p), cols(c)],
                s_xs.at[q], s_x.at[q], {"ep": z * side + o},
            ).start()

    def others(ref, q):
        return ref.at[q, pl.ds(0, (side - 1) * cap)]

    tile = min(256, half)
    per = half // tile

    def gate(q, i):
        h, at = i // per, lax.rem(i, per)
        part = pl.ds(pl.multiple_of(at * tile, tile), tile)
        x = xin[q]
        g = jnp.dot(x, wg[h, :, part], preferred_element_type=jnp.float32)
        u = jnp.dot(x, wu[h, :, part], preferred_element_type=jnp.float32)
        v = g / (1.0 + jnp.exp(-g)) * u
        hid[:, pl.ds(pl.multiple_of(i * tile, tile), tile)] = v.astype(jnp.bfloat16)

    def down(q):
        @pl.loop(0, k)
        def _(c):
            y = jnp.dot(hid[...], wd[:, cols(c)], preferred_element_type=jnp.float32)
            res[q, :, cols(c)] = y.astype(jnp.bfloat16)
            ret[q, band(p), cols(c)] = res[q, band(p), cols(c)]
            for j in range(1, side):
                o = peer(j)
                remote(
                    res.at[q, band(o), cols(c)], ret.at[q, band(p), cols(c)],
                    s_rs.at[q], s_r.at[q, c], {"ep": z * side + o},
                ).start()

    def compute(q):
        landed(others(xin, q), s_x.at[q])
        pl.loop(0, 2 * per)(lambda i: gate(q, i))
        down(q)

    def weigh(q, c):
        landed(ret.at[q, pl.ds(0, (side - 1) * cap), cols(c)], s_r.at[q, c])
        r = ret[q, :, cols(c)]
        dims = (((0,), (0,)), ((), ()))
        return lax.dot_general(
            mix[q, 0], r, dims, preferred_element_type=jnp.float32
        ) + lax.dot_general(mix[q, 1], r, dims, preferred_element_type=jnp.float32)

    def combine(q, c, add):
        t = order[q]
        y = weigh(q, c)
        to = zb if (q == 2 and add) else za
        if add:
            landed(racc.at[t, c], s_p.at[t, c])
            y = y + racc[t, c].astype(jnp.float32)
        psend[q - 1, c] = y.astype(jnp.bfloat16)
        slot = jnp.where((to == t) & (to < z), n, t)
        remote(
            psend.at[q - 1, c], racc.at[slot, c], s_ps.at[q - 1], s_p.at[slot, c], plane(to)
        ).start()

    def arrived(s, c):
        landed(tok.at[s, :, cols(c)], s_tok.at[s, c])

    @pl.loop(0, k)
    def _(c):
        disp(0, c)

    for q in range(1, n):
        landed(met.at[order[q]], s_met.at[order[q]])
        prep(q)

    def near(c):
        arrived(order[2], c)
        send_tok(order[2], c, za, 0)
        disp(2, c)

    def far(c):
        arrived(order[1], c)
        send_tok(order[1], c, zb, 1)
        disp(1, c)

    def weights():
        for i, (a, b) in enumerate(pairs):
            pltpu.make_async_copy(a, b, s_wl.at[i]).wait()
            landed(b, s_wr.at[i])

    @pl.when(mid)
    def _():
        def pass_on(c):
            arrived(order[3], c)
            send_tok(order[3], c, zb, 1)
            disp(3, c)

        for c in range(LAG):
            near(c)

        @pl.loop(LAG, k)
        def _(c):
            near(c)
            far(c - LAG)

        send_own(za, 0)
        pl.loop(k - LAG, k)(far)
        weights()
        pl.loop(0, k // 2)(pass_on)
        landed(others(xin, 1), s_x.at[1])
        turns = k - k // 2
        for j in range(turns):
            pass_on(k // 2 + j)
            for i in range(j * 2 * per // turns, (j + 1) * 2 * per // turns):
                gate(1, i)
        send_own(zb, 1)
        down(1)
        compute(2)
        compute(3)
        for c in range(LAG):
            combine(1, c, True)

        @pl.loop(LAG, k)
        def _(c):
            combine(1, c, True)
            combine(2, c - LAG, True)

        pl.loop(k - LAG, k)(lambda c: combine(2, c, True))
        compute(0)
        pl.loop(0, k)(lambda c: combine(3, c, True))

    @pl.when(end)
    def _():
        def take(c):
            arrived(order[1], c)
            disp(1, c)

        pl.loop(0, k // 2)(take)
        weights()
        compute(0)
        pl.loop(k // 2, k)(take)
        compute(1)

        @pl.loop(0, k)
        def _(c):
            arrived(order[2], c)
            disp(2, c)
            combine(1, c, False)

        compute(2)

        @pl.loop(0, k)
        def _(c):
            combine(2, c, False)
            arrived(order[3], c)
            disp(3, c)

        compute(3)
        pl.loop(0, k)(lambda c: combine(3, c, False))

    def last(c, slots):
        y = weigh(0, c)
        for slot in slots:
            landed(racc.at[slot, c], s_p.at[slot, c])
            y = y + racc[slot, c].astype(jnp.float32)
        out[:, cols(c)] = y.astype(out.dtype)

    @pl.when(end)
    def _():
        pl.loop(0, k)(lambda c: last(c, [jnp.where(z == 0, n, z)]))

    @pl.when(mid)
    def _():
        pl.loop(0, k)(lambda c: last(c, [z, n]))

    drain = landed

    for j in range(1, n):
        drain(met.at[z], s_mets.at[j - 1])
    for i, (a, b) in enumerate(pairs):
        drain(b, s_ws.at[i])
    drain(tok.at[z], s_toks.at[0, z])

    @pl.when(mid)
    def _():
        drain(tok.at[z], s_toks.at[1, z])
        drain(tok.at[z], s_toks.at[0, order[2]])
        drain(tok.at[z], s_toks.at[1, order[1]])
        drain(tok.at[z], s_toks.at[1, order[3]])

    for q in range(n):
        drain(others(snd, q), s_xs.at[q])
        drain(others(res, q), s_rs.at[q])
    for q in range(1, n):
        drain(psend.at[q - 1], s_ps.at[q - 1])


def body(
    tokens, norm_gain, norm_bias, gate_weight, up_weight, down_weight, expert_ids, route_weights
):
    count, width = tokens.shape
    experts = lax.axis_size("ep")
    cap = max(4 * count // experts, 4)
    side = experts // LINE
    half = gate_weight.shape[2]
    both = jnp.concatenate([expert_ids.astype(jnp.float32), route_weights], axis=1)
    meta = jnp.pad(both.T, ((0, 4), (0, 0)))
    rows = side * cap
    wide = width // CHUNKS
    bf = jnp.bfloat16
    dma = pltpu.SemaphoreType.DMA
    vmem = pl.BlockSpec(memory_space=pltpu.VMEM)
    hbm = pl.BlockSpec(memory_space=pl.ANY)
    return pl.pallas_call(
        functools.partial(kernel, side),
        out_shape=jax.ShapeDtypeStruct((count, width), bf),
        in_specs=[hbm, vmem, vmem] + [hbm] * 4,
        out_specs=pl.BlockSpec(memory_space=pltpu.VMEM),
        scratch_shapes=[
            pltpu.VMEM((count, width), bf),
            pltpu.VMEM((LINE, count, width), bf),
            pltpu.VMEM((LINE, 8, count), jnp.float32),
            pltpu.VMEM((2, width, half), bf),
            pltpu.VMEM((2, width, half), bf),
            pltpu.VMEM((2 * half, width), bf),
            pltpu.VMEM((LINE, rows, count), bf),
            pltpu.VMEM((LINE, 2, rows, count), bf),
            pltpu.VMEM((LINE, rows, width), bf),
            pltpu.VMEM((LINE, rows, width), bf),
            pltpu.VMEM((rows, 2 * half), bf),
            pltpu.VMEM((LINE, rows, width), bf),
            pltpu.VMEM((LINE, rows, width), bf),
            pltpu.VMEM((LINE - 1, CHUNKS, count, wide), bf),
            pltpu.VMEM((LINE + 1, CHUNKS, count, wide), bf),
            dma((2,)),
            dma((LINE,)),
            dma((LINE - 1,)),
            dma((3,)),
            dma((3,)),
            dma((3,)),
            dma((LINE, CHUNKS)),
            dma((2, LINE)),
            dma((LINE,)),
            dma((LINE,)),
            dma((LINE, CHUNKS)),
            dma((LINE,)),
            dma((LINE + 1, CHUNKS)),
            dma((LINE - 1,)),
        ],
        compiler_params=pltpu.CompilerParams(
            collective_id=0, has_side_effects=True, vmem_limit_bytes=60 * 1024 * 1024
        ),
    )(tokens, norm_gain[None], norm_bias[None], meta, gate_weight, up_weight, down_weight)


def solution(mesh):
    placed = (
        P(("ep", "tp"), None),
        P(),
        P(),
        P("ep", None, "tp"),
        P("ep", None, "tp"),
        P("ep", "tp", None),
        P(("ep", "tp"), None),
        P(("ep", "tp"), None),
    )
    return jax.shard_map(
        body, mesh=mesh, in_specs=placed, out_specs=P(("ep", "tp"), None), check_vma=False
    )
```
